32 devices in a mesh: rep: 2 (over x), fs: 8 (over z, y), tp: 2 (over core).
Axes of the slice: x: 2, y: 2, z: 4, core: 2. Of those that a mesh axis runs over, the one named last changes fastest.
Arguments:
- tokens: bfloat16 [8192, 2048], P(('rep', 'fs')), may hold values from -6 to 6
- mix_gain: float32 [2048], replicated, may hold values from 0.1 to 1.9
- gate_proj: bfloat16 [2048, 1024], P('fs', 'tp'), may hold values from -0.125 to 0.125
- value_proj: bfloat16 [2048, 1024], P('fs', 'tp'), may hold values from -0.125 to 0.125
- value_gain: float32 [1024], P('tp'), may hold values from 0.1 to 1.9
- value_shift: float32 [1024], P('tp'), may hold values from -3 to 3
- spatial_weight: bfloat16 [4, 128, 128], replicated, may hold values from -0.5 to 0.5
- spatial_shift: float32 [4, 128], replicated, may hold values from 0.1 to 1.9
- out_proj: bfloat16 [1024, 2048], P('tp', 'fs'), may hold values from -0.1875 to 0.1875
- ffn_gain: float32 [2048], replicated, may hold values from 0.1 to 1.9
- up_proj: bfloat16 [2048, 8192], P('fs', 'tp'), may hold values from -0.125 to 0.125
- down_proj: bfloat16 [8192, 2048], P('tp', 'fs'), may hold values from -0.0625 to 0.0625
Outputs:
- layer_out: bfloat16 [8192, 2048], P(('rep', 'fs'))
The draws below stay inside these ranges and needn't reach their ends.
All inputs are finite; a program needn't handle non-finite values.
Results may differ from the reference program's by a relative error of at most 0.018.
Values may be sent and summed in bfloat16 or wider, within the bound.
A program may use at most 128 MiB of HBM per device.

```python
import jax
import jax.numpy as jnp
from jax import lax

D = 2048
GW = 1024
GROUPS = 4
BLOCK = 128
FF = 8192
TOKENS = 8192
N_TP = 2


def shard_levels(stream_key, extent, cuts, low, high):
    def one(axis_at, blocks):
        heights = jax.random.uniform(jax.random.fold_in(jax.random.fold_in(stream_key, 6), axis_at), (blocks,), jnp.float32, low / len(cuts), high / len(cuts))
        return jnp.repeat(jnp.exp(heights), extent[axis_at] // blocks).reshape((-1,) + (1,) * (len(extent) - axis_at - 1))

    gain = one(*cuts[0])
    for cut in cuts[1:]:
        gain = gain * one(*cut)
    return gain


def gaussian(key, dims, width, reach, split=(), kind=jnp.bfloat16):
    entries = jax.random.normal(key, dims, jnp.float32) * width
    if len(split) > 0:
        entries = shard_levels(key, dims, split, -0.22, 0.18) * entries
    return jnp.clip(entries, min=-reach, max=reach).astype(kind)


def setup_inputs(seed: int = 0) -> dict:
    streams_of = jax.random.split(jax.random.key(seed), 13)
    return {
        "tokens": gaussian(streams_of[0], (TOKENS, D), 1.0, 6.0, ((0, 16),)),
        "mix_gain": jnp.clip(1.0 + 0.18 * jax.random.normal(streams_of[1], (D,), jnp.float32), 0.1, 1.9),
        "gate_proj": gaussian(streams_of[2], (D, GW), D ** -0.5, 0.125, ((0, 8), (1, 2))),
        "value_proj": gaussian(streams_of[3], (D, GW), D ** -0.5, 0.125, ((0, 8), (1, 2))),
        "value_gain": jnp.clip(1.0 + 0.18 * jax.random.normal(streams_of[4], (GW,), jnp.float32), 0.1, 1.9),
        "value_shift": gaussian(streams_of[5], (GW,), 0.5, 3.0, ((0, 2),), jnp.float32),
        "spatial_weight": gaussian(streams_of[6], (GROUPS, BLOCK, BLOCK), BLOCK ** -0.5, 0.5),
        "spatial_shift": jnp.clip(1.0 + 0.18 * jax.random.normal(streams_of[7], (GROUPS, BLOCK), jnp.float32), 0.1, 1.9),
        "out_proj": gaussian(streams_of[8], (GW, D), GW ** -0.5, 0.1875, ((0, 2), (1, 8))),
        "ffn_gain": jnp.clip(1.0 + 0.18 * jax.random.normal(streams_of[9], (D,), jnp.float32), 0.1, 1.9),
        "up_proj": gaussian(streams_of[10], (D, FF), D ** -0.5, 0.125, ((0, 8), (1, 2))),
        "down_proj": gaussian(streams_of[11], (FF, D), FF ** -0.5, 0.0625, ((0, 2), (1, 8))),
    }


EPS = 1e-06

def rms_norm(values, scale):
    floats = values.astype(jnp.float32)
    return (floats * lax.rsqrt(lax.optimization_barrier(jnp.mean(floats * floats, axis=-1, keepdims=True)) + EPS) * scale).astype(jnp.bfloat16)

def blocked_sum(left, right):
    rows = left.shape[0]
    inner = left.shape[1] // N_TP
    left_blocks = left.reshape(rows, N_TP, inner).transpose(1, 0, 2)
    right_blocks = right.reshape(N_TP, inner, right.shape[1])

    def step(total, pair):
        term = jnp.dot(pair[0], pair[1], preferred_element_type=jnp.float32)
        term = lax.optimization_barrier(term.astype(jnp.bfloat16)).astype(jnp.float32)
        return (total + term, None)
    start = jnp.zeros((rows, right.shape[1]), jnp.float32)
    total, unused = lax.scan(step, start, (left_blocks, right_blocks))
    return total

def reference(tokens, mix_gain, gate_proj, value_proj, value_gain, value_shift, spatial_weight, spatial_shift, out_proj, ffn_gain, up_proj, down_proj):
    rows = tokens.shape[0]
    normed = rms_norm(tokens, mix_gain)
    gate = jax.nn.gelu(jnp.dot(normed, gate_proj, preferred_element_type=jnp.float32))
    value = jax.nn.gelu(jnp.dot(normed, value_proj, preferred_element_type=jnp.float32))
    centre = lax.optimization_barrier(jnp.mean(value, axis=-1, keepdims=True))
    spread = lax.optimization_barrier(jnp.mean(value * value, axis=-1, keepdims=True)) - centre * centre
    leveled = ((value - centre) * lax.rsqrt(spread + EPS) * value_gain + value_shift).astype(jnp.bfloat16)
    lower = jnp.tril(spatial_weight).astype(jnp.float32)
    pieces = leveled.reshape(rows // BLOCK, BLOCK, GROUPS, GW // GROUPS).astype(jnp.float32)
    mixed = jnp.einsum('gts,nsgw->ntgw', lower, pieces) + spatial_shift.T[None, :, :, None]
    gated = (gate * mixed.reshape(rows, GW)).astype(jnp.bfloat16)
    midway = (tokens.astype(jnp.float32) + blocked_sum(gated, out_proj)).astype(jnp.bfloat16)
    normed2 = rms_norm(midway, ffn_gain)
    hidden = jnp.square(jax.nn.relu(jnp.dot(normed2, up_proj, preferred_element_type=jnp.float32))).astype(jnp.bfloat16)
    return (midway.astype(jnp.float32) + blocked_sum(hidden, down_proj)).astype(jnp.bfloat16)
```

```python
import jax
import jax.numpy as jnp
from jax import lax
from jax.sharding import PartitionSpec as P

GW = 1024
GROUPS = 4
BLOCK = 128
SIDE = 2


EPS = 1e-06


def rms_norm(values, scale):
    floats = values.astype(jnp.float32)
    return (
        floats * lax.rsqrt(jnp.mean(floats * floats, axis=-1, keepdims=True) + EPS) * scale
    ).astype(jnp.bfloat16)


def body(
    tokens,
    mix_gain,
    gate_proj,
    value_proj,
    value_gain,
    value_shift,
    spatial_weight,
    spatial_shift,
    out_proj,
    ffn_gain,
    up_proj,
    down_proj,
):
    normed = rms_norm(tokens, mix_gain)
    rows = normed.shape[0]
    cols = gate_proj.shape[1]
    pieces = (
        lax.all_gather(gate_proj, "fs", axis=0, tiled=True),
        lax.all_gather(value_proj, "fs", axis=0, tiled=True),
    )
    columns = normed
    gate_acc = jnp.dot(columns, pieces[0], preferred_element_type=jnp.float32)
    value_acc = jnp.dot(columns, pieces[1], preferred_element_type=jnp.float32)
    gate = jax.nn.gelu(gate_acc)
    value = jax.nn.gelu(value_acc)
    sums, squares = lax.psum((jnp.sum(value, axis=-1), jnp.sum(value * value, axis=-1)), "tp")
    centre = (sums / GW)[:, None]
    spread = (squares / GW)[:, None] - centre * centre
    leveled = ((value - centre) * lax.rsqrt(spread + EPS) * value_gain + value_shift).astype(
        jnp.bfloat16
    )
    group_width = GW // GROUPS
    span = min(cols, group_width)
    count = cols // span
    first = lax.axis_index("tp") * cols // group_width
    lower = jnp.tril(lax.dynamic_slice_in_dim(spatial_weight, first, count, 0))
    offsets = lax.dynamic_slice_in_dim(spatial_shift, first, count, 0)
    pieces = leveled.reshape(rows // BLOCK, BLOCK, count, span)
    mixed = (
        jnp.einsum("gts,nsgw->ntgw", lower, pieces, preferred_element_type=jnp.float32)
        + offsets.T[None, :, :, None]
    )
    gated = (gate * mixed.reshape(rows, cols)).astype(jnp.bfloat16)
    out_whole = lax.all_gather(out_proj, "fs", axis=1, tiled=True)
    mixer_terms = jnp.dot(gated, out_whole, preferred_element_type=jnp.float32)
    mixer_total = lax.psum(mixer_terms.astype(jnp.bfloat16), "tp").astype(jnp.float32)
    midway = (tokens.astype(jnp.float32) + mixer_total).astype(jnp.bfloat16)
    normed2 = rms_norm(midway, ffn_gain)
    columns = normed2
    hidden_acc = jnp.dot(
        columns,
        lax.all_gather(up_proj, "fs", axis=0, tiled=True),
        preferred_element_type=jnp.float32,
    )
    hidden = jnp.square(jax.nn.relu(hidden_acc)).astype(jnp.bfloat16)
    down_whole = lax.all_gather(down_proj, "fs", axis=1, tiled=True)
    ffn_terms = jnp.dot(hidden, down_whole, preferred_element_type=jnp.float32)
    ffn_total = lax.psum(ffn_terms.astype(jnp.bfloat16), "tp").astype(jnp.float32)
    return (midway.astype(jnp.float32) + ffn_total).astype(jnp.bfloat16)

def fast_body(shape, args):
    (
        tokens,
        mix_gain,
        gate_proj,
        value_proj,
        value_gain,
        value_shift,
        spatial_weight,
        spatial_shift,
        out_proj,
        ffn_gain,
        up_proj,
        down_proj,
    ) = args
    f32, bf16 = jnp.float32, jnp.bfloat16
    reps, shards, cores = shape["rep"], shape["fs"], shape["tp"]
    depth = shards // SIDE
    rep, fs, core = lax.axis_index("rep"), lax.axis_index("fs"), lax.axis_index("tp")
    layer, side = fs // SIDE, fs % SIDE
    members = reps * SIDE

    def over_x(a):
        return lax.ppermute(a, "rep", [(i, reps - 1 - i) for i in range(reps)])

    def over_y(a):
        return lax.ppermute(a, "fs", [(i, i ^ 1) for i in range(shards)])

    def over_xy(a):
        pairs = [
            (i * shards + j, (reps - 1 - i) * shards + (j ^ 1))
            for i in range(reps)
            for j in range(shards)
        ]
        return lax.ppermute(a, ("rep", "fs"), pairs)

    def over_z(a):
        return lax.ppermute(a, "fs", [(i, (i + SIDE) % shards) for i in range(shards)])

    def over_core(a):
        return lax.ppermute(a, "tp", [(i, cores - 1 - i) for i in range(cores)])

    def after(a, *others):
        return lax.optimization_barrier((a,) + others)[0]

    def in_order(mine, other, axis):
        first = jnp.where(side == 0, mine, other)
        second = jnp.where(side == 0, other, mine)
        return jnp.concatenate([first, second], axis)

    def dot(a, b):
        return jnp.dot(a, b, preferred_element_type=f32)

    half_rows = out_proj.shape[0] // reps
    carried = jnp.where(rep == 0, gate_proj, value_proj)
    out_half = lax.dynamic_slice_in_dim(out_proj, rep * half_rows, half_rows, 0)
    carried_other, out_other = over_y(carried), over_y(out_half)
    packed = jnp.concatenate(
        [in_order(carried, carried_other, 0), in_order(out_half, out_other, 1)], 0
    )
    width = SIDE * gate_proj.shape[0]

    slab = up_proj.shape[1] // members

    def up_slab(r, s):
        return lax.dynamic_slice_in_dim(up_proj, (r * SIDE + s) * slab, slab, 1)

    def down_slab(r, s):
        return lax.dynamic_slice_in_dim(down_proj, (r * SIDE + s) * slab, slab, 0)

    up_other = over_y(after(up_slab(rep, 1 - side), carried_other, out_other))
    up_block = in_order(up_slab(rep, side), up_other, 0)
    down_other = over_y(after(down_slab(rep, 1 - side), up_other))
    down_block = in_order(down_slab(rep, side), down_other, 1)

    mix_ring = [packed]
    for step in range(depth - 1):
        mix_ring.append(over_z(mix_ring[-1]))
    up_ring = [after(up_block, *mix_ring[-2:-1])]
    for step in range(depth - 1):
        up_ring.append(over_z(up_ring[-1]))
    down_ring = [after(down_block, *up_ring[-2:-1])]
    for step in range(depth - 1):
        down_ring.append(over_z(down_ring[-1]))

    rows = tokens.shape[0] // cores

    def ring_order(a):
        starts = [((layer - k) % depth) * width for k in range(depth)]
        return jnp.concatenate(
            [lax.dynamic_slice_in_dim(a, s, width, a.ndim - 1) for s in starts], a.ndim - 1
        )

    own = ring_order(lax.dynamic_slice_in_dim(tokens, core * rows, rows, 0))
    normed = rms_norm(own, ring_order(mix_gain))
    mine_acc, other_acc = [0.0, 0.0], [0.0, 0.0]
    outs = []
    for k in range(depth):
        mine = mix_ring[k]
        other = over_x(mine)
        pairs = ((mine, other), (over_core(mine), over_core(other)))
        columns = normed[:, k * width : (k + 1) * width]
        for h in range(cores):
            mine_acc[h] = mine_acc[h] + dot(columns, pairs[h][0][:width])
            other_acc[h] = other_acc[h] + dot(columns, pairs[h][1][:width])
        outs.append([[m[width:] for m in pairs[h]] for h in range(cores)])
    mine_acc, other_acc = jnp.concatenate(mine_acc, 1), jnp.concatenate(other_acc, 1)
    gate = jax.nn.gelu(jnp.where(rep == 0, mine_acc, other_acc))
    value = jax.nn.gelu(jnp.where(rep == 0, other_acc, mine_acc))
    centre = jnp.mean(value, axis=-1, keepdims=True)
    spread = jnp.mean(value * value, axis=-1, keepdims=True) - centre * centre
    gain = jnp.concatenate([value_gain, over_core(value_gain)])
    shift = jnp.concatenate([value_shift, over_core(value_shift)])
    leveled = ((value - centre) * lax.rsqrt(spread + EPS) * gain + shift).astype(bf16)

    blocks = rows // BLOCK
    row_at = lax.broadcasted_iota(jnp.int32, (rows, rows), 0)
    col_at = lax.broadcasted_iota(jnp.int32, (rows, rows), 1)
    keep = (row_at >= col_at) & (row_at // BLOCK == col_at // BLOCK)
    span = GW // GROUPS
    per_core = GROUPS // cores
    gated = []
    for h in range(cores):
        owner = core if h == 0 else cores - 1 - core
        parts = []
        for i in range(per_core):
            at = owner * per_core + i
            lo = (h * per_core + i) * span
            matrix = lax.dynamic_index_in_dim(spatial_weight, at, 0, False)
            matrix = jnp.where(keep, jnp.tile(matrix, (blocks, blocks)), 0)
            offset = jnp.tile(lax.dynamic_index_in_dim(spatial_shift, at, 0, False), blocks)
            mixed = dot(matrix.astype(bf16), leveled[:, lo : lo + span]) + offset[:, None]
            parts.append((gate[:, lo : lo + span] * mixed).astype(bf16))
        gated.append(
            (jnp.where(rep == 0, parts[0], parts[1]), jnp.where(rep == 0, parts[1], parts[0]))
        )
    mixer = []
    for k in range(depth):
        total = 0.0
        for h in range(cores):
            for i in range(reps):
                total = total + dot(gated[h][i], outs[k][h][i])
        mixer.append(total)
    midway = (own.astype(f32) + jnp.concatenate(mixer, 1)).astype(bf16)
    normed2 = rms_norm(midway, ring_order(ffn_gain))

    cut = rows // 2
    top, bottom = normed2[:cut], normed2[cut:]
    top_x, bottom_y = over_x(top), over_y(bottom)
    top_y, bottom_x = over_y(top), over_x(bottom)
    top_xy, bottom_xy = over_y(top_x), over_x(bottom_y)
    plane = jnp.concatenate(
        [normed2, top_x, bottom_x, top_y, bottom_y, top_xy, bottom_xy], 0
    )
    up_mine = jnp.concatenate(up_ring, 0)
    up_sibling = jnp.concatenate([over_core(u) for u in up_ring], 0)
    hidden = [
        jnp.square(jax.nn.relu(dot(plane, u))).astype(bf16) for u in (up_mine, up_sibling)
    ]
    finals = []
    for k in range(depth):
        mine = down_ring[k]
        part = (dot(hidden[0], mine) + dot(hidden[1], over_core(mine))).astype(bf16)
        total = part[:rows].astype(f32)
        for n, send in enumerate((over_x, over_y, over_xy)):
            total = total + send(part[(n + 1) * rows : (n + 2) * rows]).astype(f32)
        final = (midway[:, k * width : (k + 1) * width].astype(f32) + total).astype(bf16)
        sibling = over_core(final)
        finals.append(
            jnp.concatenate(
                [jnp.where(core == 0, final, sibling), jnp.where(core == 0, sibling, final)], 0
            )
        )
    circle = jnp.concatenate(finals[::-1] + finals[::-1], 1)
    return lax.dynamic_slice_in_dim(
        circle, (depth - 1 - layer) * width, depth * width, 1
    )


def solution(mesh):
    shape = dict(mesh.shape)

    def step(*args):
        rows = args[0].shape[0]
        fits = shape["rep"] == 2 and shape["tp"] == 2 and shape["fs"] % SIDE == 0
        if fits and rows % (shape["tp"] * BLOCK) == 0:
            return fast_body(shape, args)
        return body(*args)

    return jax.shard_map(
        step,
        mesh=mesh,
        in_specs=(
            P(("rep", "fs"), None),
            P(),
            P("fs", "tp"),
            P("fs", "tp"),
            P("tp"),
            P("tp"),
            P(),
            P(),
            P("tp", "fs"),
            P(),
            P("fs", "tp"),
            P("tp", "fs"),
        ),
        out_specs=P(("rep", "fs"), None),
        check_vma=False,
    )
```

```python
import jax
import jax.numpy as jnp
from jax import lax
from jax.sharding import PartitionSpec as P


GW = 1024
GROUPS = 4
BLOCK = 128
SIDE = 2


EPS = 1e-06


def rms_norm(values, scale):
    floats = values.astype(jnp.float32)
    return (
        floats * lax.rsqrt(jnp.mean(floats * floats, axis=-1, keepdims=True) + EPS) * scale
    ).astype(jnp.bfloat16)


def body(
    tokens,
    mix_gain,
    gate_proj,
    value_proj,
    value_gain,
    value_shift,
    spatial_weight,
    spatial_shift,
    out_proj,
    ffn_gain,
    up_proj,
    down_proj,
):
    normed = rms_norm(tokens, mix_gain)
    rows = normed.shape[0]
    cols = gate_proj.shape[1]
    pieces = (
        lax.all_gather(gate_proj, "fs", axis=0, tiled=True),
        lax.all_gather(value_proj, "fs", axis=0, tiled=True),
    )
    columns = normed
    gate_acc = jnp.dot(columns, pieces[0], preferred_element_type=jnp.float32)
    value_acc = jnp.dot(columns, pieces[1], preferred_element_type=jnp.float32)
    gate = jax.nn.gelu(gate_acc)
    value = jax.nn.gelu(value_acc)
    sums, squares = lax.psum((jnp.sum(value, axis=-1), jnp.sum(value * value, axis=-1)), "tp")
    centre = (sums / GW)[:, None]
    spread = (squares / GW)[:, None] - centre * centre
    leveled = ((value - centre) * lax.rsqrt(spread + EPS) * value_gain + value_shift).astype(
        jnp.bfloat16
    )
    group_width = GW // GROUPS
    span = min(cols, group_width)
    count = cols // span
    first = lax.axis_index("tp") * cols // group_width
    lower = jnp.tril(lax.dynamic_slice_in_dim(spatial_weight, first, count, 0))
    offsets = lax.dynamic_slice_in_dim(spatial_shift, first, count, 0)
    pieces = leveled.reshape(rows // BLOCK, BLOCK, count, span)
    mixed = (
        jnp.einsum("gts,nsgw->ntgw", lower, pieces, preferred_element_type=jnp.float32)
        + offsets.T[None, :, :, None]
    )
    gated = (gate * mixed.reshape(rows, cols)).astype(jnp.bfloat16)
    out_whole = lax.all_gather(out_proj, "fs", axis=1, tiled=True)
    mixer_terms = jnp.dot(gated, out_whole, preferred_element_type=jnp.float32)
    mixer_total = lax.psum(mixer_terms.astype(jnp.bfloat16), "tp").astype(jnp.float32)
    midway = (tokens.astype(jnp.float32) + mixer_total).astype(jnp.bfloat16)
    normed2 = rms_norm(midway, ffn_gain)
    columns = normed2
    hidden_acc = jnp.dot(
        columns,
        lax.all_gather(up_proj, "fs", axis=0, tiled=True),
        preferred_element_type=jnp.float32,
    )
    hidden = jnp.square(jax.nn.relu(hidden_acc)).astype(jnp.bfloat16)
    down_whole = lax.all_gather(down_proj, "fs", axis=1, tiled=True)
    ffn_terms = jnp.dot(hidden, down_whole, preferred_element_type=jnp.float32)
    ffn_total = lax.psum(ffn_terms.astype(jnp.bfloat16), "tp").astype(jnp.float32)
    return (midway.astype(jnp.float32) + ffn_total).astype(jnp.bfloat16)


def fast_body(shape, args):
    (
        tokens,
        mix_gain,
        gate_proj,
        value_proj,
        value_gain,
        value_shift,
        spatial_weight,
        spatial_shift,
        out_proj,
        ffn_gain,
        up_proj,
        down_proj,
    ) = args
    f32, bf16 = jnp.float32, jnp.bfloat16
    reps, shards, cores = shape["rep"], shape["fs"], shape["tp"]
    depth = shards // SIDE
    rep, fs, core = lax.axis_index("rep"), lax.axis_index("fs"), lax.axis_index("tp")
    layer, side = fs // SIDE, fs % SIDE
    members = reps * SIDE

    def over_x(a):
        return lax.ppermute(a, "rep", [(i, reps - 1 - i) for i in range(reps)])

    def over_y(a):
        return lax.ppermute(a, "fs", [(i, i ^ 1) for i in range(shards)])

    def over_xy(a):
        pairs = [
            (i * shards + j, (reps - 1 - i) * shards + (j ^ 1))
            for i in range(reps)
            for j in range(shards)
        ]
        return lax.ppermute(a, ("rep", "fs"), pairs)

    def over_z(a, k, layers=None):
        pairs = [(i, i ^ (k * SIDE)) for i in range(shards)]
        return lax.ppermute(
            a, "fs", [p for p in pairs if layers is None or p[0] // SIDE in layers]
        )

    middle = (1, depth - 2)

    inner = (layer == middle[0]) | (layer == middle[1])

    def over_z3(a):
        return over_z(a, 3, middle)

    def relay(second):
        return over_z(second, 1, middle)

    def over_core(a):
        return lax.ppermute(a, "tp", [(i, cores - 1 - i) for i in range(cores)])

    def after(a, *others):
        return lax.optimization_barrier((a,) + others)[0]

    def in_order(mine, other, axis):
        first = jnp.where(side == 0, mine, other)
        second = jnp.where(side == 0, other, mine)
        return jnp.concatenate([first, second], axis)

    def dot(a, b):
        return jnp.dot(a, b, preferred_element_type=f32)

    half_rows = out_proj.shape[0] // reps
    in_width = gate_proj.shape[1]
    carried = jnp.where(rep == 0, gate_proj, value_proj)
    out_half = lax.dynamic_slice_in_dim(out_proj, rep * half_rows, half_rows, 0)
    packed = jnp.concatenate([carried, out_half], 1)
    width = SIDE * gate_proj.shape[0]
    mix_blocks = [packed] + [over_z(packed, k) for k in range(1, depth)]

    slab = up_proj.shape[1] // members

    def up_slab(r, s):
        return lax.dynamic_slice_in_dim(up_proj, (r * SIDE + s) * slab, slab, 1)

    def down_slab(r, s):
        return lax.dynamic_slice_in_dim(down_proj, (r * SIDE + s) * slab, slab, 0)

    up_other = over_y(up_slab(rep, 1 - side))
    up_block = in_order(up_slab(rep, side), up_other, 0)
    up_second = over_z(up_block, 2)
    up_first = over_z(up_block, 1)
    up_third = over_z3(up_block)

    rows = tokens.shape[0] // cores

    def ring_order(a):
        starts = [(layer ^ k) * width for k in range(depth)]
        return jnp.concatenate(
            [lax.dynamic_slice_in_dim(a, s, width, a.ndim - 1) for s in starts], a.ndim - 1
        )

    own = ring_order(lax.dynamic_slice_in_dim(tokens, core * rows, rows, 0))
    normed = rms_norm(own, ring_order(mix_gain))
    mine_acc, other_acc = [0.0, 0.0], [0.0, 0.0]
    outs = []
    for k in range(depth):
        mine = mix_blocks[k] if k == 0 else after(mix_blocks[k], up_other)
        across_x = over_x(mine)
        across_y = over_y(mine)
        across_xy = over_y(across_x) if k == 2 else over_x(across_y)
        pairs = ((mine, across_y), (across_x, across_xy))
        block = jnp.concatenate(
            [in_order(m[:, :in_width], o[:, :in_width], 0) for m, o in pairs]
            + [in_order(m[:, in_width:], o[:, in_width:], 1) for m, o in pairs],
            0,
        )
        columns = normed[:, k * width : (k + 1) * width]
        halves = (block, over_core(block))
        for h in range(cores):
            mine_acc[h] = mine_acc[h] + dot(columns, halves[h][:width])
            other_acc[h] = other_acc[h] + dot(columns, halves[h][width : 2 * width])
        outs.append([m[2 * width :] for m in halves])
    down_other = over_y(after(down_slab(rep, 1 - side), across_x, across_y))
    down_block = in_order(down_slab(rep, side), down_other, 1)
    mine_acc, other_acc = jnp.concatenate(mine_acc, 1), jnp.concatenate(other_acc, 1)
    gate = jax.nn.gelu(jnp.where(rep == 0, mine_acc, other_acc))
    value = jax.nn.gelu(jnp.where(rep == 0, other_acc, mine_acc))
    centre = jnp.mean(value, axis=-1, keepdims=True)
    spread = jnp.mean(value * value, axis=-1, keepdims=True) - centre * centre
    gain = jnp.concatenate([value_gain, over_core(value_gain)])
    shift = jnp.concatenate([value_shift, over_core(value_shift)])
    leveled = ((value - centre) * lax.rsqrt(spread + EPS) * gain + shift).astype(bf16)

    blocks = rows // BLOCK
    row_at = lax.broadcasted_iota(jnp.int32, (rows, rows), 0)
    col_at = lax.broadcasted_iota(jnp.int32, (rows, rows), 1)
    keep = (row_at >= col_at) & (row_at // BLOCK == col_at // BLOCK)
    span = GW // GROUPS
    per_core = GROUPS // cores
    gated = []
    for h in range(cores):
        owner = core if h == 0 else cores - 1 - core
        parts = []
        for i in range(per_core):
            at = owner * per_core + i
            lo = (h * per_core + i) * span
            matrix = lax.dynamic_index_in_dim(spatial_weight, at, 0, False)
            matrix = jnp.where(keep, jnp.tile(matrix, (blocks, blocks)), 0)
            offset = jnp.tile(lax.dynamic_index_in_dim(spatial_shift, at, 0, False), blocks)
            mixed = dot(matrix.astype(bf16), leveled[:, lo : lo + span]) + offset[:, None]
            parts.append((gate[:, lo : lo + span] * mixed).astype(bf16))
        gated.append(
            jnp.concatenate(
                [jnp.where(rep == 0, parts[0], parts[1]), jnp.where(rep == 0, parts[1], parts[0])],
                1,
            )
        )
    mixer = []
    for k in range(depth):
        total = 0.0
        for h in range(cores):
            total = total + dot(gated[h], outs[k][h])
        mixer.append(total)
    midway = (own.astype(f32) + jnp.concatenate(mixer, 1)).astype(bf16)
    normed2 = rms_norm(midway, ring_order(ffn_gain))

    up_relayed = relay(after(up_second, normed2))
    down_ready = after(down_block, normed2)
    down_second = over_z(down_ready, 2)
    down_third = over_z3(down_ready)
    down_first = over_z(down_ready, 1)
    up_blocks = [up_block, up_first, up_second, jnp.where(inner, up_third, up_relayed)]

    cut = rows // 2
    top, bottom = normed2[:cut], normed2[cut:]
    top_x, bottom_y = over_x(top), over_y(bottom)
    top_y, bottom_x = over_y(top), over_x(bottom)
    top_xy, bottom_xy = over_y(top_x), over_x(bottom_y)
    plane = jnp.concatenate(
        [normed2, top_x, bottom_x, top_y, bottom_y, top_xy, bottom_xy], 0
    )
    hidden = []
    for move in (lambda u: u, over_core):
        up_columns = jnp.concatenate([move(u) for u in up_blocks], 0)
        hidden.append(jnp.square(jax.nn.relu(dot(plane, up_columns))).astype(bf16))
    out = jnp.zeros(tokens.shape, bf16)
    part = total = None
    for k in (0, 2, 1, 3):
        if k == 0:
            mine = down_block
        elif k == 2:
            down_relayed = relay(after(down_second, part))
            mine = after(down_second, total)
        elif k == 1:
            mine = after(down_first, total)
        else:
            mine = jnp.where(inner, down_third, after(down_relayed, total))
        part = (dot(hidden[0], mine) + dot(hidden[1], over_core(mine))).astype(bf16)
        total = part[:rows].astype(f32)
        for n, send in enumerate((over_x, over_y, over_xy)):
            total = total + send(part[(n + 1) * rows : (n + 2) * rows]).astype(f32)
        final = (midway[:, k * width : (k + 1) * width].astype(f32) + total).astype(bf16)
        sibling = over_core(final)
        both = jnp.concatenate(
            [jnp.where(core == 0, final, sibling), jnp.where(core == 0, sibling, final)], 0
        )
        out = lax.dynamic_update_slice_in_dim(out, both, (layer ^ k) * width, 1)
    return out


def solution(mesh):
    shape = dict(mesh.shape)

    def step(*args):
        rows = args[0].shape[0]
        fits = shape["rep"] == 2 and shape["tp"] == 2 and shape["fs"] == 4 * SIDE
        if fits and rows % (shape["tp"] * BLOCK) == 0:
            return fast_body(shape, args)
        return body(*args)

    return jax.shard_map(
        step,
        mesh=mesh,
        in_specs=(
            P(("rep", "fs"), None),
            P(),
            P("fs", "tp"),
            P("fs", "tp"),
            P("tp"),
            P("tp"),
            P(),
            P(),
            P("tp", "fs"),
            P(),
            P("fs", "tp"),
            P("tp", "fs"),
        ),
        out_specs=P(("rep", "fs"), None),
        check_vma=False,
    )
```

```python
import jax
import jax.numpy as jnp
from jax import lax
from jax.sharding import PartitionSpec as P


GW = 1024
GROUPS = 4
BLOCK = 128
SIDE = 2


EPS = 1e-06


def rms_norm(values, scale):
    floats = values.astype(jnp.float32)
    return (
        floats * lax.rsqrt(jnp.mean(floats * floats, axis=-1, keepdims=True) + EPS) * scale
    ).astype(jnp.bfloat16)


def body(
    tokens,
    mix_gain,
    gate_proj,
    value_proj,
    value_gain,
    value_shift,
    spatial_weight,
    spatial_shift,
    out_proj,
    ffn_gain,
    up_proj,
    down_proj,
):
    normed = rms_norm(tokens, mix_gain)
    rows = normed.shape[0]
    cols = gate_proj.shape[1]
    pieces = (
        lax.all_gather(gate_proj, "fs", axis=0, tiled=True),
        lax.all_gather(value_proj, "fs", axis=0, tiled=True),
    )
    columns = normed
    gate_acc = jnp.dot(columns, pieces[0], preferred_element_type=jnp.float32)
    value_acc = jnp.dot(columns, pieces[1], preferred_element_type=jnp.float32)
    gate = jax.nn.gelu(gate_acc)
    value = jax.nn.gelu(value_acc)
    sums, squares = lax.psum((jnp.sum(value, axis=-1), jnp.sum(value * value, axis=-1)), "tp")
    centre = (sums / GW)[:, None]
    spread = (squares / GW)[:, None] - centre * centre
    leveled = ((value - centre) * lax.rsqrt(spread + EPS) * value_gain + value_shift).astype(
        jnp.bfloat16
    )
    group_width = GW // GROUPS
    span = min(cols, group_width)
    count = cols // span
    first = lax.axis_index("tp") * cols // group_width
    lower = jnp.tril(lax.dynamic_slice_in_dim(spatial_weight, first, count, 0))
    offsets = lax.dynamic_slice_in_dim(spatial_shift, first, count, 0)
    pieces = leveled.reshape(rows // BLOCK, BLOCK, count, span)
    mixed = (
        jnp.einsum("gts,nsgw->ntgw", lower, pieces, preferred_element_type=jnp.float32)
        + offsets.T[None, :, :, None]
    )
    gated = (gate * mixed.reshape(rows, cols)).astype(jnp.bfloat16)
    out_whole = lax.all_gather(out_proj, "fs", axis=1, tiled=True)
    mixer_terms = jnp.dot(gated, out_whole, preferred_element_type=jnp.float32)
    mixer_total = lax.psum(mixer_terms.astype(jnp.bfloat16), "tp").astype(jnp.float32)
    midway = (tokens.astype(jnp.float32) + mixer_total).astype(jnp.bfloat16)
    normed2 = rms_norm(midway, ffn_gain)
    columns = normed2
    hidden_acc = jnp.dot(
        columns,
        lax.all_gather(up_proj, "fs", axis=0, tiled=True),
        preferred_element_type=jnp.float32,
    )
    hidden = jnp.square(jax.nn.relu(hidden_acc)).astype(jnp.bfloat16)
    down_whole = lax.all_gather(down_proj, "fs", axis=1, tiled=True)
    ffn_terms = jnp.dot(hidden, down_whole, preferred_element_type=jnp.float32)
    ffn_total = lax.psum(ffn_terms.astype(jnp.bfloat16), "tp").astype(jnp.float32)
    return (midway.astype(jnp.float32) + ffn_total).astype(jnp.bfloat16)


def fast_body(shape, args):
    (
        tokens,
        mix_gain,
        gate_proj,
        value_proj,
        value_gain,
        value_shift,
        spatial_weight,
        spatial_shift,
        out_proj,
        ffn_gain,
        up_proj,
        down_proj,
    ) = args
    f32, bf16 = jnp.float32, jnp.bfloat16
    reps, shards, cores = shape["rep"], shape["fs"], shape["tp"]
    depth = shards // SIDE
    rep, fs, core = lax.axis_index("rep"), lax.axis_index("fs"), lax.axis_index("tp")
    layer, side = fs // SIDE, fs % SIDE
    members = reps * SIDE

    def over_x(a):
        return lax.ppermute(a, "rep", [(i, reps - 1 - i) for i in range(reps)])

    def over_y(a):
        return lax.ppermute(a, "fs", [(i, i ^ 1) for i in range(shards)])

    def over_xy(a):
        pairs = [
            (i * shards + j, (reps - 1 - i) * shards + (j ^ 1))
            for i in range(reps)
            for j in range(shards)
        ]
        return lax.ppermute(a, ("rep", "fs"), pairs)

    def over_z(a, k, layers=None):
        pairs = [(i, i ^ (k * SIDE)) for i in range(shards)]
        return lax.ppermute(
            a, "fs", [p for p in pairs if layers is None or p[0] // SIDE in layers]
        )

    middle = (1, depth - 2)

    inner = (layer == middle[0]) | (layer == middle[1])

    def over_z3(a):
        return over_z(a, 3, middle)

    def relay(second):
        return over_z(second, 1, middle)

    def over_core(a):
        return lax.ppermute(a, "tp", [(i, cores - 1 - i) for i in range(cores)])

    def after(a, *others):
        return lax.optimization_barrier((a,) + others)[0]

    def in_order(mine, other, axis):
        first = jnp.where(side == 0, mine, other)
        second = jnp.where(side == 0, other, mine)
        return jnp.concatenate([first, second], axis)

    def dot(a, b):
        return jnp.dot(a, b, preferred_element_type=f32)

    half_rows = out_proj.shape[0] // reps
    in_width = gate_proj.shape[1]
    carried = jnp.where(rep == 0, gate_proj, value_proj)
    out_half = lax.dynamic_slice_in_dim(out_proj, rep * half_rows, half_rows, 0)
    packed = jnp.concatenate([carried, out_half], 1)
    width = SIDE * gate_proj.shape[0]
    mix_blocks = [packed] + [over_z(packed, k) for k in range(1, depth)]

    slab = up_proj.shape[1] // members

    def up_slab(r, s):
        return lax.dynamic_slice_in_dim(up_proj, (r * SIDE + s) * slab, slab, 1)

    def down_slab(r, s):
        return lax.dynamic_slice_in_dim(down_proj, (r * SIDE + s) * slab, slab, 0)

    up_other = over_y(up_slab(rep, 1 - side))
    up_block = in_order(up_slab(rep, side), up_other, 0)
    up_second = over_z(up_block, 2)
    up_first = over_z(up_block, 1)
    up_third = over_z3(up_block)

    rows = tokens.shape[0] // cores

    def ring_order(a):
        starts = [(layer ^ k) * width for k in range(depth)]
        return jnp.concatenate(
            [lax.dynamic_slice_in_dim(a, s, width, a.ndim - 1) for s in starts], a.ndim - 1
        )

    own = ring_order(lax.dynamic_slice_in_dim(tokens, core * rows, rows, 0))
    normed = rms_norm(own, ring_order(mix_gain))
    mine_acc, other_acc = [0.0, 0.0], [0.0, 0.0]
    outs = []
    for k in range(depth):
        mine = mix_blocks[k] if k == 0 else after(mix_blocks[k], up_other)
        across_x = over_x(mine)
        across_y = over_y(mine)
        across_xy = over_y(across_x) if k == 2 else over_x(across_y)
        pairs = ((mine, across_y), (across_x, across_xy))
        block = jnp.concatenate(
            [in_order(m[:, :in_width], o[:, :in_width], 0) for m, o in pairs]
            + [in_order(m[:, in_width:], o[:, in_width:], 1) for m, o in pairs],
            0,
        )
        columns = normed[:, k * width : (k + 1) * width]
        halves = (block, over_core(block))
        for h in range(cores):
            mine_acc[h] = mine_acc[h] + dot(columns, halves[h][:width])
            other_acc[h] = other_acc[h] + dot(columns, halves[h][width : 2 * width])
        outs.append([m[2 * width :] for m in halves])
    down_other = over_y(after(down_slab(rep, 1 - side), across_x, across_y))
    down_block = in_order(down_slab(rep, side), down_other, 1)
    mine_acc, other_acc = jnp.concatenate(mine_acc, 1), jnp.concatenate(other_acc, 1)
    gate = jax.nn.gelu(jnp.where(rep == 0, mine_acc, other_acc))
    value = jax.nn.gelu(jnp.where(rep == 0, other_acc, mine_acc))
    centre = jnp.mean(value, axis=-1, keepdims=True)
    spread = jnp.mean(value * value, axis=-1, keepdims=True) - centre * centre
    gain = jnp.concatenate([value_gain, over_core(value_gain)])
    shift = jnp.concatenate([value_shift, over_core(value_shift)])
    leveled = ((value - centre) * lax.rsqrt(spread + EPS) * gain + shift).astype(bf16)

    blocks = rows // BLOCK
    row_at = lax.broadcasted_iota(jnp.int32, (rows, rows), 0)
    col_at = lax.broadcasted_iota(jnp.int32, (rows, rows), 1)
    keep = (row_at >= col_at) & (row_at // BLOCK == col_at // BLOCK)
    span = GW // GROUPS
    per_core = GROUPS // cores
    gated = []
    for h in range(cores):
        owner = core if h == 0 else cores - 1 - core
        parts = []
        for i in range(per_core):
            at = owner * per_core + i
            lo = (h * per_core + i) * span
            matrix = lax.dynamic_index_in_dim(spatial_weight, at, 0, False)
            matrix = jnp.where(keep, jnp.tile(matrix, (blocks, blocks)), 0)
            offset = jnp.tile(lax.dynamic_index_in_dim(spatial_shift, at, 0, False), blocks)
            mixed = dot(matrix.astype(bf16), leveled[:, lo : lo + span]) + offset[:, None]
            parts.append((gate[:, lo : lo + span] * mixed).astype(bf16))
        gated.append(
            jnp.concatenate(
                [jnp.where(rep == 0, parts[0], parts[1]), jnp.where(rep == 0, parts[1], parts[0])],
                1,
            )
        )
    mixer = []
    for k in range(depth):
        total = 0.0
        for h in range(cores):
            total = total + dot(gated[h], outs[k][h])
        mixer.append(total)
    midway = (own.astype(f32) + jnp.concatenate(mixer, 1)).astype(bf16)
    normed2 = rms_norm(midway, ring_order(ffn_gain))

    up_relayed = relay(after(up_second, normed2))
    down_ready = after(down_block, normed2)
    down_second = over_z(down_ready, 2)
    down_third = over_z3(down_ready)
    down_first = over_z(down_ready, 1)
    up_blocks = [up_block, up_first, up_second, jnp.where(inner, up_third, up_relayed)]

    cut = rows // 2
    top, bottom = normed2[:cut], normed2[cut:]
    top_x, bottom_y = over_x(top), over_y(bottom)
    top_y, bottom_x = over_y(top), over_x(bottom)
    top_xy, bottom_xy = over_y(top_x), over_x(bottom_y)
    plane = jnp.concatenate(
        [normed2, top_x, bottom_x, top_y, bottom_y, top_xy, bottom_xy], 0
    )
    hidden = []
    for move in (lambda u: u, over_core):
        up_columns = jnp.concatenate([move(u) for u in up_blocks], 0)
        hidden.append(jnp.square(jax.nn.relu(dot(plane, up_columns))).astype(bf16))
    out = jnp.zeros(tokens.shape, bf16)
    part = total = None
    for k in (0, 2, 1, 3):
        if k == 0:
            mine = down_block
        elif k == 2:
            down_relayed = relay(after(down_second, part))
            mine = after(down_second, total)
        elif k == 1:
            mine = after(down_first, total)
        else:
            mine = jnp.where(inner, down_third, after(down_relayed, arrived[0]))
        part = (dot(hidden[0], mine) + dot(hidden[1], over_core(mine))).astype(bf16)
        total = part[:rows].astype(f32)
        arrived = [
            send(part[(n + 1) * rows : (n + 2) * rows])
            for n, send in enumerate((over_x, over_y, over_xy))
        ]
        for term in arrived:
            total = total + term.astype(f32)
        final = (midway[:, k * width : (k + 1) * width].astype(f32) + total).astype(bf16)
        sibling = over_core(final)
        both = jnp.concatenate(
            [jnp.where(core == 0, final, sibling), jnp.where(core == 0, sibling, final)], 0
        )
        out = lax.dynamic_update_slice_in_dim(out, both, (layer ^ k) * width, 1)
    return out


def solution(mesh):
    shape = dict(mesh.shape)

    def step(*args):
        rows = args[0].shape[0]
        fits = shape["rep"] == 2 and shape["tp"] == 2 and shape["fs"] == 4 * SIDE
        if fits and rows % (shape["tp"] * BLOCK) == 0:
            return fast_body(shape, args)
        return body(*args)

    return jax.shard_map(
        step,
        mesh=mesh,
        in_specs=(
            P(("rep", "fs"), None),
            P(),
            P("fs", "tp"),
            P("fs", "tp"),
            P("tp"),
            P("tp"),
            P(),
            P(),
            P("tp", "fs"),
            P(),
            P("fs", "tp"),
            P("tp", "fs"),
        ),
        out_specs=P(("rep", "fs"), None),
        check_vma=False,
    )
```
